32 devices in a mesh: sp: 16 (over z, y, x), tp: 2 (over core).
Axes of the slice: x: 2, y: 2, z: 4, core: 2. Of those that a mesh axis runs over, the one named last changes fastest.
Arguments:
- tokens: bfloat16 [4096, 2048], P('sp', 'tp'), may hold values from -12 to 12
- norm_gain: float32 [2048], replicated, may hold values from 0.1 to 1.9
- window_query: bfloat16 [2048, 1024], P(None, 'tp'), may hold values from -2 to 2
- window_key: bfloat16 [2048, 512], P(None, 'tp'), may hold values from -2 to 2
- window_value: bfloat16 [2048, 512], P(None, 'tp'), may hold values from -0.125 to 0.125
- window_gate: bfloat16 [2048, 1024], P(None, 'tp'), may hold values from -0.125 to 0.125
- window_sink: float32 [16], P('tp'), may hold values from 2 to 6
- pair_query: bfloat16 [2048, 1024], P(None, 'tp'), may hold values from -2 to 2
- pair_key: bfloat16 [2048, 1024], P(None, 'tp'), may hold values from -2 to 2
- pair_value: bfloat16 [2048, 1024], P(None, 'tp'), may hold values from -0.125 to 0.125
- pair_gate: bfloat16 [2048, 1024], P(None, 'tp'), may hold values from -0.125 to 0.125
- map_lambda: float32 [8], P('tp'), may hold values from 0.3 to 0.8
- head_gain: float32 [128], replicated, may hold values from 0.1 to 1.9
- window_out: bfloat16 [1024, 2048], P('tp'), may hold values from -0.125 to 0.125
- pair_out: bfloat16 [1024, 2048], P('tp'), may hold values from -0.125 to 0.125
Outputs:
- mixed: bfloat16 [4096, 2048], P(('sp', 'tp'))
The draws below stay inside these ranges and needn't reach their ends.
All inputs are finite; a program needn't handle non-finite values.
Results may differ from the reference program's by a relative error of at most 0.018.
Values may be sent and summed in bfloat16 or wider, within the bound.
A program may use at most 128 MiB of HBM per device.

```python
import math
import jax
import jax.numpy as jnp
from jax import lax

D = 2048
HD = 64
A_HEADS = 16
A_KV = 8
B_HEADS = 8
WINDOW = 128
SEQ = 4096
HEAD_GROUPS = 2


def base_weight(key, noise_tag, columns, fan_in):
    noise = jax.random.normal(jax.random.fold_in(key, noise_tag), (D, columns), jnp.float32)
    return jnp.clip(noise, -6.0, 6.0) * fan_in ** (-0.5)


def draw_tokens(key, part):
    values = jnp.clip(jax.random.normal(jax.random.fold_in(key, 21), (SEQ, D), jnp.float32), -6.0, 6.0)
    return values.astype(jnp.bfloat16)


def draw_window_query(key, part):
    weight = base_weight(key, 31, A_HEADS * HD, D)
    return weight.astype(jnp.bfloat16)


def draw_window_key(key, part):
    weight = base_weight(key, 32, A_KV * HD, D)
    return weight.astype(jnp.bfloat16)


def draw_pair_query(key, part):
    weight = base_weight(key, 33, B_HEADS * 2 * HD, D // 2)
    return weight.astype(jnp.bfloat16)


def draw_pair_key(key, part):
    weight = base_weight(key, 34, B_HEADS * 2 * HD, D // 2)
    return weight.astype(jnp.bfloat16)


def shard_levels(own_key, extent, pieces, least, top_value):
    def one(axis_at, parts):
        draws = jax.random.uniform(jax.random.fold_in(jax.random.fold_in(own_key, 6), axis_at), (parts,), jnp.float32, least / len(pieces), top_value / len(pieces))
        return jnp.repeat(jnp.exp(draws), extent[axis_at] // parts).reshape((-1,) + (1,) * (len(extent) - axis_at - 1))

    gain = one(*pieces[0])
    for cut in pieces[1:]:
        gain = gain * one(*cut)
    return gain


def gaussian(rng, shape, scale, bound, pieces=(), kind=jnp.bfloat16):
    loudness = shard_levels(rng, shape, pieces, -0.22, 0.18) if pieces else 1.0
    values = jax.random.normal(rng, shape, jnp.float32) * scale * loudness
    return jnp.minimum(jnp.maximum(values, -bound), bound).astype(kind)


def setup_inputs(seed: int = 0) -> dict:
    key_list = jax.random.split(jax.random.key(seed), 16)
    tokens = draw_tokens(jax.random.fold_in(key_list[15], 71), 0)
    norm_gain = jnp.clip(1.0 + 0.18 * jax.random.normal(key_list[1], (D,), jnp.float32), 0.1, 1.9)
    window_query = draw_window_query(jax.random.fold_in(key_list[15], 71), 0)
    window_key = draw_window_key(jax.random.fold_in(key_list[15], 71), 0)
    window_value = gaussian(key_list[4], (D, A_KV * HD), D ** -0.5, 0.125, ((1, 2),))
    window_gate = gaussian(key_list[5], (D, A_HEADS * HD), D ** -0.5, 0.125, ((1, 2),))
    window_sink = jnp.clip(2.0 + 4.0 * jax.random.uniform(key_list[6], (A_HEADS,), jnp.float32) ** shard_levels(key_list[6], (A_HEADS,), ((0, 2),), -0.2, 0.2), 2.0, 6.0)
    pair_query = draw_pair_query(jax.random.fold_in(key_list[15], 71), 0)
    pair_key = draw_pair_key(jax.random.fold_in(key_list[15], 71), 0)
    pair_value = gaussian(key_list[9], (D, B_HEADS * 2 * HD), D ** -0.5, 0.125, ((1, 2),))
    pair_gate = gaussian(key_list[10], (D, B_HEADS * 2 * HD), D ** -0.5, 0.125, ((1, 2),))
    map_lambda = jnp.clip(0.3 + 0.5 * jax.random.uniform(key_list[11], (B_HEADS,), jnp.float32) ** shard_levels(key_list[11], (B_HEADS,), ((0, 2),), -0.2, 0.2), 0.3, 0.8)
    head_gain = jnp.clip(1.0 + 0.18 * jax.random.normal(key_list[12], (2 * HD,), jnp.float32), 0.1, 1.9)
    window_out = gaussian(key_list[13], (A_HEADS * HD, D), (A_HEADS * HD + 2 * B_HEADS * HD) ** -0.5, 0.125, ((0, 2),))
    pair_out = gaussian(key_list[14], (2 * B_HEADS * HD, D), (A_HEADS * HD + 2 * B_HEADS * HD) ** -0.5, 0.125, ((0, 2),))
    return dict(tokens=tokens, norm_gain=norm_gain, window_query=window_query, window_key=window_key, window_value=window_value, window_gate=window_gate, window_sink=window_sink, pair_query=pair_query, pair_key=pair_key, pair_value=pair_value, pair_gate=pair_gate, map_lambda=map_lambda, head_gain=head_gain, window_out=window_out, pair_out=pair_out)


norm_eps = 1e-06
head_scale = 0.8

def row_norm(values, gain_vec):
    squares = lax.optimization_barrier(jnp.mean(values * values, axis=-1, keepdims=True))
    return values * lax.rsqrt(squares + norm_eps) * gain_vec

def reference(tokens, norm_gain, window_query, window_key, window_value, window_gate, window_sink, pair_query, pair_key, pair_value, pair_gate, map_lambda, head_gain, window_out, pair_out):
    seq_len = tokens.shape[0]
    normed = row_norm(tokens.astype(jnp.float32), norm_gain).astype(jnp.bfloat16)

    def project(weight):
        return jnp.dot(normed.astype(jnp.float32), weight.astype(jnp.float32), preferred_element_type=jnp.float32).astype(jnp.bfloat16)
    slide_query = project(window_query)
    slide_key = project(window_key)
    slide_value = project(window_value)
    slide_gate = project(window_gate)
    paired_query = project(pair_query)
    paired_key = project(pair_key)
    paired_value = project(pair_value)
    paired_gate = project(pair_gate)
    scale = HD ** (-0.5)
    group_size = A_HEADS // A_KV
    blocks_count = seq_len // WINDOW
    queries = slide_query.reshape(blocks_count, WINDOW, A_KV, group_size, HD).astype(jnp.float32)

    def band(values):
        before = jnp.pad(values, ((WINDOW, 0), (0, 0)))[:seq_len]
        return jnp.concatenate([before.reshape(blocks_count, WINDOW, A_KV, HD), values.reshape(blocks_count, WINDOW, A_KV, HD)], axis=1).astype(jnp.float32)
    band_keys = band(slide_key)
    band_values = band(slide_value)
    sink_logit = window_sink.reshape(A_KV, group_size)[:, :, None, None]
    query_idx = jnp.arange(WINDOW, dtype=jnp.int32)[:, None]
    key_idx = jnp.arange(2 * WINDOW, dtype=jnp.int32)[None, :]
    distance = query_idx - key_idx + WINDOW

    def window_block(inputs):
        block_query, block_keys, block_values, block_number = inputs
        scores = jnp.einsum('ikgd,jkd->kgij', block_query, block_keys) * scale
        valid = (distance >= 0) & (distance < WINDOW) & (block_number * WINDOW - WINDOW + key_idx >= 0)
        masked = jnp.where(valid, scores, -jnp.inf)
        top = jnp.maximum(lax.optimization_barrier(jnp.max(masked, axis=-1, keepdims=True)), sink_logit)
        weights = jnp.where(valid, jnp.exp(masked - top), 0.0)
        probs = weights / (lax.optimization_barrier(jnp.sum(weights, axis=-1, keepdims=True)) + jnp.exp(sink_logit - top))
        probs = lax.optimization_barrier(probs.astype(jnp.bfloat16)).astype(jnp.float32)
        return jnp.einsum('kgij,jkd->ikgd', probs, block_values)
    slide_out = lax.map(window_block, (queries, band_keys, band_values, jnp.arange(blocks_count, dtype=jnp.int32)))
    slide_out = slide_out.reshape(seq_len, A_HEADS * HD)
    slide_mix = (slide_out * jax.nn.silu(slide_gate.astype(jnp.float32))).astype(jnp.bfloat16)
    q_block = math.gcd(seq_len, 256)
    pair_queries = paired_query.reshape(seq_len, B_HEADS, 2, HD).astype(jnp.float32)
    pair_keys = paired_key.reshape(seq_len, B_HEADS, 2, HD).astype(jnp.float32)
    pair_values = paired_value.reshape(seq_len, B_HEADS, 2 * HD).astype(jnp.float32)
    key_pos = jnp.arange(seq_len, dtype=jnp.int32)

    def pair_block(block_number):
        begin = block_number * q_block
        block_query = lax.dynamic_slice_in_dim(pair_queries, begin, q_block, 0)
        query_pos = begin + jnp.arange(q_block, dtype=jnp.int32)
        scores = jnp.einsum('ihcd,jhcd->hcij', block_query, pair_keys) * scale
        causal = query_pos[:, None] >= key_pos[None, :]
        masked = jnp.where(causal, scores, -jnp.inf)
        top = lax.optimization_barrier(jnp.max(masked, axis=-1, keepdims=True))
        weights = jnp.where(causal, jnp.exp(masked - top), 0.0)
        totals = lax.optimization_barrier(jnp.sum(weights, axis=-1))
        rounded = lax.optimization_barrier(weights.astype(jnp.bfloat16)).astype(jnp.float32)
        numer = jnp.einsum('hcij,jhe->hcie', rounded, pair_values)
        return numer / totals[..., None]
    per_map = lax.map(pair_block, jnp.arange(seq_len // q_block, dtype=jnp.int32))
    differ = per_map[:, :, 0] - map_lambda[None, :, None, None] * per_map[:, :, 1]
    head_out = row_norm(differ, head_gain) * head_scale
    head_out = jnp.transpose(head_out, (0, 2, 1, 3)).reshape(seq_len, B_HEADS, 2 * HD)
    gate_act = jax.nn.silu(paired_gate.astype(jnp.float32).reshape(seq_len, B_HEADS, 2 * HD))
    paired_mix = (head_out * gate_act).reshape(seq_len, B_HEADS * 2 * HD).astype(jnp.bfloat16)
    slide_cols = A_HEADS * HD // HEAD_GROUPS
    paired_cols = B_HEADS * 2 * HD // HEAD_GROUPS
    total = jnp.zeros((seq_len, D), jnp.float32)
    for group_index in range(HEAD_GROUPS):
        slide_part = slide_mix[:, group_index * slide_cols:(group_index + 1) * slide_cols]
        paired_part = paired_mix[:, group_index * paired_cols:(group_index + 1) * paired_cols]
        partial_sum = jnp.dot(slide_part.astype(jnp.float32), window_out[group_index * slide_cols:(group_index + 1) * slide_cols].astype(jnp.float32), preferred_element_type=jnp.float32)
        partial_sum = partial_sum + jnp.dot(paired_part.astype(jnp.float32), pair_out[group_index * paired_cols:(group_index + 1) * paired_cols].astype(jnp.float32), preferred_element_type=jnp.float32)
        total = total + lax.optimization_barrier(partial_sum.astype(jnp.bfloat16)).astype(jnp.float32)
    return total.astype(jnp.bfloat16)
```

```python
import functools
import math

import jax
import jax.numpy as jnp
from jax import lax
from jax.experimental import pallas as pl
from jax.experimental.pallas import tpu as pltpu
from jax.sharding import PartitionSpec as P

HD = 64
WINDOW = 128

norm_eps = 1e-06
head_scale = 0.8

MESH = pl.DeviceIdType.MESH
F32 = jnp.float32
BF16 = jnp.bfloat16


def dot_nt(a, b):
    return lax.dot_general(a, b, (((1,), (1,)), ((), ())), preferred_element_type=F32)


def dot_tn(a, b):
    return lax.dot_general(a, b, (((0,), (0,)), ((), ())), preferred_element_type=F32)


def silu(v):
    return v / (1.0 + jnp.exp(-v))


def kernel(
    S,
    T,
    tokens,
    norm_gain,
    wq_h,
    wk_h,
    wv_h,
    wg_h,
    sink,
    pq_h,
    pk_h,
    pv_h,
    pg_h,
    lam,
    head_gain,
    wo_h,
    po_h,
    out,
    wq,
    wk,
    wv,
    wg,
    pq,
    pk,
    pv,
    pg,
    wo,
    po,
    tok_buf,
    normed,
    band_k,
    band_v,
    sq_buf,
    sg_buf,
    pg_buf,
    slide_mix,
    paired_mix,
    kv_send,
    q_send,
    kv_all,
    q_all,
    q2_buf,
    m_buf,
    l_buf,
    acc_buf,
    ret_send,
    ret_all,
    part,
    part_bf,
    rs_buf,
    w_sem,
    tok_s,
    tok_r,
    kv1_s,
    kv2_s,
    kv_r,
    q_s,
    q_r,
    tail_s,
    tail_r,
    ret_s,
    ret_r,
    rs_s,
    rs_r,
):
    R = tokens.shape[0]
    Dl = tokens.shape[1]
    D = Dl * T
    G = kv_send.shape[0]
    M = S // G
    C = kv_send.shape[3]
    Hg = C // (2 * HD)
    s = lax.axis_index("sp")
    t = lax.axis_index("tp")
    g = s // M
    m = lax.rem(s, M)

    pairs = [(pk_h, pk), (pv_h, pv), (pq_h, pq), (wk_h, wk), (wv_h, wv), (wq_h, wq), (wg_h, wg), (pg_h, pg), (wo_h, wo), (po_h, po)]
    loads = [pltpu.make_async_copy(a, b, w_sem.at[i]) for i, (a, b) in enumerate(pairs)]
    for cp in loads:
        cp.start()

    barrier = pltpu.get_barrier_semaphore()
    for dt in range(1, T):
        pl.semaphore_signal(barrier, inc=1, device_id={"tp": lax.rem(t + dt, T)}, device_id_type=MESH)

    def greet(d, _):
        pl.semaphore_signal(barrier, inc=1, device_id={"sp": lax.rem(s + d, S)}, device_id_type=MESH)
        return 0

    lax.fori_loop(1, S, greet, 0)
    tok_buf[t] = tokens[...]
    pl.semaphore_wait(barrier, S + T - 2)

    def tok_copy(dt):
        return pltpu.make_async_remote_copy(
            tokens,
            tok_buf.at[t],
            tok_s.at[dt],
            tok_r.at[dt],
            device_id={"tp": lax.rem(t + dt, T)},
            device_id_type=MESH,
        )

    def tok_in(dt):
        return pltpu.make_async_remote_copy(
            tokens,
            tok_buf.at[lax.rem(t + T - dt, T)],
            tok_s.at[dt],
            tok_r.at[dt],
            device_id={"tp": lax.rem(t + dt, T)},
            device_id_type=MESH,
        )

    for dt in range(1, T):
        tok_copy(dt).start()
    for dt in range(1, T):
        tok_in(dt).wait_recv()

    NB = 32

    def norm_rows(i, _):
        rows = pl.ds(pl.multiple_of(i * NB, NB), NB)
        xs = [tok_buf[k, rows, :].astype(F32) for k in range(T)]
        total = sum(jnp.sum(x * x, axis=-1, keepdims=True) for x in xs)
        r = lax.rsqrt(total * (1.0 / D) + norm_eps)
        for k in range(T):
            cols = slice(k * Dl, (k + 1) * Dl)
            normed[rows, cols] = (xs[k] * r * norm_gain[:, cols]).astype(BF16)
        return 0

    lax.fori_loop(0, R // NB, norm_rows, 0)

    def project(i, store):
        loads[i].wait()
        w = pairs[i][1]
        cols = w.shape[1]
        tile = min(256, cols)
        for c in range(0, cols, tile):
            r = jnp.dot(normed[...], w[:, c : c + tile], preferred_element_type=F32).astype(BF16)
            store(c, tile, r)

    def grouped(write):
        def store(c, tile, r):
            for o in range(0, tile, 2 * HD):
                at = c + o
                write(at // C, at % C, r[:, o : o + 2 * HD])

        return store

    def put_k(gi, col, r):
        kv_send[gi, 0, :, col : col + 2 * HD] = r

    def put_v(gi, col, r):
        kv_send[gi, 1, :, col : col + 2 * HD] = r

    def put_q(gi, col, r):
        q_send[gi, :, col : col + 2 * HD] = r

    def plane(gi, mi):
        return {"sp": gi * M + mi}

    def kv1(dg):
        return pltpu.make_async_remote_copy(
            kv_send.at[lax.rem(g + dg, G)],
            kv_all.at[s],
            kv1_s.at[dg],
            kv_r.at[dg * M],
            device_id=plane(lax.rem(g + dg, G), m),
            device_id_type=MESH,
        )

    def source(dg, dm):
        return lax.rem(g + G - dg, G) * M + lax.rem(m + M - dm, M)

    def kv_in(dg, dm):
        at = kv_all.at[source(dg, dm)]
        return pltpu.make_async_remote_copy(
            at,
            at,
            kv2_s.at[dg * M + dm],
            kv_r.at[dg * M + dm],
            device_id=plane(g, lax.rem(m + 1, M)),
            device_id_type=MESH,
        )

    def kv2(dg, dm):
        at = kv_all.at[source(dg, 0)]
        return pltpu.make_async_remote_copy(
            at,
            at,
            kv2_s.at[dg * M + dm],
            kv_r.at[dg * M + dm],
            device_id=plane(g, lax.rem(m + dm, M)),
            device_id_type=MESH,
        )

    def forward(dg):
        def one(dm, _):
            kv2(dg, dm).start()
            return 0

        lax.fori_loop(1, M, one, 0)

    def q_copy(dg):
        return pltpu.make_async_remote_copy(
            q_send.at[lax.rem(g + dg, G)],
            q_all.at[g],
            q_s.at[dg],
            q_r.at[dg],
            device_id=plane(lax.rem(g + dg, G), m),
            device_id_type=MESH,
        )

    def q_in(dg):
        return pltpu.make_async_remote_copy(
            q_send.at[0],
            q_all.at[lax.rem(g + G - dg, G)],
            q_s.at[dg],
            q_r.at[dg],
            device_id=plane(lax.rem(g + dg, G), m),
            device_id_type=MESH,
        )

    project(0, grouped(put_k))
    project(1, grouped(put_v))
    for dg in range(1, G):
        kv1(dg).start()
    kv_all[s] = kv_send[g]
    forward(0)
    project(2, grouped(put_q))
    for dg in range(1, G):
        q_copy(dg).start()
    q_all[g] = q_send[g]

    def into(ref, first=0):
        def store(c, tile, r):
            ref[first:, c : c + tile] = r

        return store

    project(3, into(band_k, WINDOW))
    project(4, into(band_v, WINDOW))

    def tails():
        nxt = {"sp": lax.rem(s + 1, S)}
        return [
            pltpu.make_async_remote_copy(
                b.at[pl.ds(R, WINDOW)],
                b.at[pl.ds(0, WINDOW)],
                tail_s.at[i],
                tail_r.at[i],
                device_id=nxt,
                device_id_type=MESH,
            )
            for i, b in enumerate((band_k, band_v))
        ]

    @pl.when(s < S - 1)
    def _():
        for cp in tails():
            cp.start()

    @pl.when(s == 0)
    def _():
        band_k[0:WINDOW] = jnp.zeros((WINDOW, band_k.shape[1]), BF16)
        band_v[0:WINDOW] = jnp.zeros((WINDOW, band_v.shape[1]), BF16)

    def relay(dg):
        if dg < G:
            kv_in(dg, 0).wait_recv()
            forward(dg)

    project(5, into(sq_buf))
    project(6, into(sg_buf))
    relay(1)
    project(7, into(pg_buf))
    relay(2)

    @pl.when(s > 0)
    def _():
        for cp in tails():
            cp.wait_recv()

    scale = HD**-0.5
    kv_heads = band_k.shape[1] // HD
    group = sq_buf.shape[1] // band_k.shape[1]
    W = WINDOW
    blocks = R // W
    key_i = lax.broadcasted_iota(jnp.int32, (2 * W, group * W), 0)
    qry_i = lax.rem(lax.broadcasted_iota(jnp.int32, (2 * W, group * W), 1), W)
    lane_head = lax.broadcasted_iota(jnp.int32, (1, group * W), 1) // W
    dist = qry_i - key_i + W
    in_band = (dist >= 0) & (dist < W)

    def window_block(b):
        r0 = b * W
        ok = in_band & (s * R + r0 - W + key_i >= 0)
        for h in range(kv_heads):
            k = band_k[r0 : r0 + 2 * W, h * HD : (h + 1) * HD]
            v = band_v[r0 : r0 + 2 * W, h * HD : (h + 1) * HD]
            q = jnp.concatenate(
                [sq_buf[r0 : r0 + W, (h * group + e) * HD : (h * group + e + 1) * HD] for e in range(group)], axis=0
            )
            sc = jnp.where(ok, dot_nt(k, q) * scale, -jnp.inf)
            sk = jnp.full((1, group * W), sink[0, h * group], F32)
            for e in range(1, group):
                sk = jnp.where(lane_head == e, sink[0, h * group + e], sk)
            top = jnp.maximum(jnp.max(sc, axis=0, keepdims=True), sk)
            w = jnp.exp(sc - top)
            den = jnp.sum(w, axis=0, keepdims=True) + jnp.exp(sk - top)
            probs = (w * (1.0 / den)).astype(BF16)
            o = dot_tn(v, probs)
            o = jnp.concatenate([o[:, e * W : (e + 1) * W] for e in range(group)], axis=0).T
            cols = slice(h * group * HD, (h + 1) * group * HD)
            gate = sg_buf[r0 : r0 + W, cols].astype(F32)
            slide_mix[r0 : r0 + W, cols] = (o * silu(gate)).astype(BF16)

    for b in range(blocks):
        window_block(b)
        if b == 0:
            relay(3)
    for dg in range(4, G):
        relay(dg)

    for dg in range(1, G):
        q_in(dg).wait_recv()
    lane = lax.broadcasted_iota(jnp.int32, (R, 2 * HD), 1)
    for gi in range(G):
        for j in range(Hg):
            q = q_all[gi, :, j * 2 * HD : (j + 1) * 2 * HD].astype(F32) * scale
            q2_buf[gi, j, 0:R, :] = jnp.where(lane < HD, q, 0.0).astype(BF16)
            q2_buf[gi, j, R:, :] = jnp.where(lane < HD, 0.0, q).astype(BF16)
    m_buf[...] = jnp.full(m_buf.shape, -1e30, F32)
    l_buf[...] = jnp.zeros(l_buf.shape, F32)
    acc_buf[...] = jnp.zeros(acc_buf.shape, F32)

    def update(at, gi, masked):
        for j in range(Hg):
            cols = slice(j * 2 * HD, (j + 1) * 2 * HD)
            st = dot_nt(kv_all[at, 0, :, cols], q2_buf[gi, j])
            if masked:
                ki = lax.broadcasted_iota(jnp.int32, (R, 2 * R), 0)
                qi = lax.rem(lax.broadcasted_iota(jnp.int32, (R, 2 * R), 1), R)
                st = jnp.where(qi >= ki, st, -jnp.inf)
            old = m_buf[gi, j]
            new = jnp.maximum(old, jnp.max(st, axis=0, keepdims=True))
            f = jnp.exp(old - new)
            p = jnp.exp(st - new)
            m_buf[gi, j] = new
            l_buf[gi, j] = l_buf[gi, j] * f + jnp.sum(p, axis=0, keepdims=True)
            acc_buf[gi, j] = acc_buf[gi, j] * f + dot_tn(kv_all[at, 1, :, cols], p.astype(BF16))

    def process(at):
        def one(gi, _):
            mine = gi * M + m

            @pl.when(at < mine)
            def _():
                update(at, gi, False)

            @pl.when(at == mine)
            def _():
                update(at, gi, True)

            return 0

        lax.fori_loop(0, G, one, 0)

    def near(dg, _):
        process(source(dg, 0))
        return 0

    lax.fori_loop(0, G, near, 0)

    def far(i, _):
        dg = i // (M - 1)
        dm = 1 + lax.rem(i, M - 1)
        kv_in(dg, dm).wait_recv()
        process(source(dg, dm))
        return 0

    if M > 1:
        lax.fori_loop(0, G * (M - 1), far, 0)

    def ret_copy(dg):
        return pltpu.make_async_remote_copy(
            ret_send.at[lax.rem(g + dg, G)],
            ret_all.at[g],
            ret_s.at[dg],
            ret_r.at[dg],
            device_id=plane(lax.rem(g + dg, G), m),
            device_id_type=MESH,
        )

    def ret_in(dg):
        return pltpu.make_async_remote_copy(
            ret_send.at[0],
            ret_all.at[lax.rem(g + G - dg, G)],
            ret_s.at[dg],
            ret_r.at[dg],
            device_id=plane(lax.rem(g + dg, G), m),
            device_id_type=MESH,
        )

    def finish(gi):
        for j in range(Hg):
            a = acc_buf[gi, j] * (1.0 / l_buf[gi, j])
            d = a[:, 0:R] - lam[0, g * Hg + j] * a[:, R:]
            sq = jnp.mean(d * d, axis=0, keepdims=True)
            y = (d * (lax.rsqrt(sq + norm_eps) * head_scale)).T * head_gain[...]
            ret_send[gi, :, j * 2 * HD : (j + 1) * 2 * HD] = y.astype(BF16)

    for dg in range(1, G):
        finish(lax.rem(g + dg, G))
        ret_copy(dg).start()
    finish(g)
    ret_all[g] = ret_send[g]

    loads[8].wait()
    NT = min(512, D)
    for c in range(0, D, NT):
        part[:, c : c + NT] = jnp.dot(slide_mix[...], wo[:, c : c + NT], preferred_element_type=F32)
    for dg in range(1, G):
        ret_in(dg).wait_recv()
    for gi in range(G):
        gate = pg_buf[:, gi * C : (gi + 1) * C].astype(F32)
        paired_mix[:, gi * C : (gi + 1) * C] = (ret_all[gi].astype(F32) * silu(gate)).astype(BF16)
    loads[9].wait()
    Rt = R // T
    for c in range(0, D, NT):
        r = part[:, c : c + NT] + jnp.dot(paired_mix[...], po[:, c : c + NT], preferred_element_type=F32)
        r = r.astype(BF16)
        for k in range(T):
            part_bf[k, :, c : c + NT] = r[k * Rt : (k + 1) * Rt]

    def rs_copy(dt):
        return pltpu.make_async_remote_copy(
            part_bf.at[lax.rem(t + dt, T)],
            rs_buf.at[dt],
            rs_s.at[dt],
            rs_r.at[dt],
            device_id={"tp": lax.rem(t + dt, T)},
            device_id_type=MESH,
        )

    for dt in range(1, T):
        rs_copy(dt).start()
    for dt in range(1, T):
        rs_copy(dt).wait_recv()
    for c in range(0, D, NT):
        total = part_bf[t, :, c : c + NT].astype(F32)
        for dt in range(1, T):
            total = total + rs_buf[dt, :, c : c + NT].astype(F32)
        out[:, c : c + NT] = total.astype(BF16)

    for dt in range(1, T):
        tok_copy(dt).wait_send()
        rs_copy(dt).wait_send()
    for dg in range(1, G):
        kv1(dg).wait_send()
        q_copy(dg).wait_send()
        ret_copy(dg).wait_send()

    def drain(i, _):
        kv2(i // (M - 1), 1 + lax.rem(i, M - 1)).wait_send()
        return 0

    if M > 1:
        lax.fori_loop(0, G * (M - 1), drain, 0)

    @pl.when(s < S - 1)
    def _():
        for cp in tails():
            cp.wait_send()


def per_device(S, T, tokens, norm_gain, wq, wk, wv, wg, sink, pq, pk, pv, pg, lam, head_gain, wo, po):
    R, Dl = tokens.shape
    D = Dl * T
    A = wq.shape[1]
    KC = wk.shape[1]
    B = pq.shape[1]
    H = B // (2 * HD)
    G = math.gcd(H, S)
    Hg = H // G
    C = Hg * 2 * HD
    vmem = pl.BlockSpec(memory_space=pltpu.VMEM)
    smem = pl.BlockSpec(memory_space=pltpu.SMEM)
    hbm = pl.BlockSpec(memory_space=pl.ANY)
    dma = pltpu.SemaphoreType.DMA
    V = pltpu.VMEM
    scratch = [V(w.shape, BF16) for w in (wq, wk, wv, wg, pq, pk, pv, pg, wo, po)]
    scratch += [
        V((T, R, Dl), BF16),
        V((R, D), BF16),
        V((WINDOW + R, KC), BF16),
        V((WINDOW + R, KC), BF16),
        V((R, A), BF16),
        V((R, A), BF16),
        V((R, B), BF16),
        V((R, A), BF16),
        V((R, B), BF16),
        V((G, 2, R, C), BF16),
        V((G, R, C), BF16),
        V((S, 2, R, C), BF16),
        V((G, R, C), BF16),
        V((G, Hg, 2 * R, 2 * HD), BF16),
        V((G, Hg, 1, 2 * R), F32),
        V((G, Hg, 1, 2 * R), F32),
        V((G, Hg, 2 * HD, 2 * R), F32),
        V((G, R, C), BF16),
        V((G, R, C), BF16),
        V((R, D), F32),
        V((T, R // T, D), BF16),
        V((T, R // T, D), BF16),
        dma((10,)),
        dma((T,)),
        dma((T,)),
        dma((G,)),
        dma((S,)),
        dma((S,)),
        dma((G,)),
        dma((G,)),
        dma((2,)),
        dma((2,)),
        dma((G,)),
        dma((G,)),
        dma((T,)),
        dma((T,)),
    ]
    return pl.pallas_call(
        functools.partial(kernel, S, T),
        out_shape=jax.ShapeDtypeStruct((R // T, D), BF16),
        in_specs=[vmem, vmem, hbm, hbm, hbm, hbm, smem, hbm, hbm, hbm, hbm, smem, vmem, hbm, hbm],
        out_specs=vmem,
        scratch_shapes=scratch,
        compiler_params=pltpu.CompilerParams(
            collective_id=0, has_side_effects=True, vmem_limit_bytes=60 * 1024 * 1024
        ),
        name="layer",
    )(
        tokens,
        norm_gain.reshape(1, D),
        wq,
        wk,
        wv,
        wg,
        sink.reshape(1, -1),
        pq,
        pk,
        pv,
        pg,
        lam.reshape(1, -1),
        head_gain.reshape(1, -1),
        wo,
        po,
    )


def solution(mesh):
    S, T = mesh.shape["sp"], mesh.shape["tp"]
    in_specs = (
        P("sp", "tp"),
        P(),
        P(None, "tp"),
        P(None, "tp"),
        P(None, "tp"),
        P(None, "tp"),
        P("tp"),
        P(None, "tp"),
        P(None, "tp"),
        P(None, "tp"),
        P(None, "tp"),
        P("tp"),
        P(),
        P("tp", None),
        P("tp", None),
    )
    return jax.shard_map(
        functools.partial(per_device, S, T),
        mesh=mesh,
        in_specs=in_specs,
        out_specs=P(("sp", "tp"), None),
        check_vma=False,
    )
```

```python
import functools
import math

import jax
import jax.numpy as jnp
from jax import lax
from jax.experimental import pallas as pl
from jax.experimental.pallas import tpu as pltpu
from jax.sharding import PartitionSpec as P

HD = 64
WINDOW = 128

norm_eps = 1e-06
head_scale = 0.8

MESH = pl.DeviceIdType.MESH
F32 = jnp.float32
BF16 = jnp.bfloat16


def dot_nt(a, b):
    return lax.dot_general(a, b, (((1,), (1,)), ((), ())), preferred_element_type=F32)


def dot_tn(a, b):
    return lax.dot_general(a, b, (((0,), (0,)), ((), ())), preferred_element_type=F32)


def silu(v):
    return v / (1.0 + jnp.exp(-v))


def kernel(
    S,
    T,
    tokens,
    norm_gain,
    wq_h,
    wk_h,
    wv_h,
    wg_h,
    sink,
    pq_h,
    pk_h,
    pv_h,
    pg_h,
    lam,
    head_gain,
    wo_h,
    po_h,
    out,
    wq,
    wk,
    wv,
    wg,
    pq,
    pk,
    pv,
    pg,
    wo,
    po,
    tok_buf,
    normed,
    band_k,
    band_v,
    sq_buf,
    sg_buf,
    pg_buf,
    slide_mix,
    paired_mix,
    kv_send,
    q_send,
    kv_all,
    q_all,
    q2_buf,
    m_buf,
    l_buf,
    acc_buf,
    ret_send,
    ret_all,
    part,
    part_bf,
    w_sem,
    tok_s,
    tok_r,
    kv1_s,
    kv2_s,
    kv_r,
    q_s,
    q_r,
    tail_s,
    tail_r,
    ret_s,
    ret_r,
    rs_s,
    rs_r,
):
    R = tokens.shape[0]
    Dl = tokens.shape[1]
    D = Dl * T
    G = kv_send.shape[0]
    M = S // G
    C = kv_send.shape[3]
    Hg = C // (2 * HD)
    s = lax.axis_index("sp")
    t = lax.axis_index("tp")
    g = s // M
    m = lax.rem(s, M)

    pairs = [(pq_h, pq), (pk_h, pk), (pv_h, pv), (wk_h, wk), (wv_h, wv), (wq_h, wq), (wg_h, wg), (pg_h, pg), (wo_h, wo), (po_h, po)]
    loads = [pltpu.make_async_copy(a, b, w_sem.at[i]) for i, (a, b) in enumerate(pairs)]
    for cp in loads:
        cp.start()

    barrier = pltpu.get_barrier_semaphore()
    for dt in range(1, T):
        pl.semaphore_signal(barrier, inc=1, device_id={"tp": lax.rem(t + dt, T)}, device_id_type=MESH)

    def greet(d, _):
        pl.semaphore_signal(barrier, inc=1, device_id={"sp": lax.rem(s + d, S)}, device_id_type=MESH)
        return 0

    lax.fori_loop(1, S, greet, 0)
    tok_buf[t] = tokens[...]
    pl.semaphore_wait(barrier, S + T - 2)

    TC = tok_s.shape[1]
    CR = R // TC

    def tok_copy(dt, i):
        return pltpu.make_async_remote_copy(
            tokens.at[pl.ds(i * CR, CR)],
            tok_buf.at[t, pl.ds(i * CR, CR)],
            tok_s.at[dt, i],
            tok_r.at[dt, i],
            device_id={"tp": lax.rem(t + dt, T)},
            device_id_type=MESH,
        )

    def tok_in(dt, i):
        return pltpu.make_async_remote_copy(
            tokens.at[pl.ds(i * CR, CR)],
            tok_buf.at[lax.rem(t + T - dt, T), pl.ds(i * CR, CR)],
            tok_s.at[dt, i],
            tok_r.at[dt, i],
            device_id={"tp": lax.rem(t + dt, T)},
            device_id_type=MESH,
        )

    for i in range(TC):
        for dt in range(1, T):
            tok_copy(dt, i).start()

    NB = 32

    def norm_rows(i, _):
        rows = pl.ds(pl.multiple_of(i * NB, NB), NB)
        xs = [tok_buf[k, rows, :].astype(F32) for k in range(T)]
        total = sum(jnp.sum(x * x, axis=-1, keepdims=True) for x in xs)
        r = lax.rsqrt(total * (1.0 / D) + norm_eps)
        for k in range(T):
            cols = slice(k * Dl, (k + 1) * Dl)
            normed[rows, cols] = (xs[k] * r * norm_gain[:, cols]).astype(BF16)
        return 0

    for i in range(TC):
        for dt in range(1, T):
            tok_in(dt, i).wait_recv()
        lax.fori_loop(i * CR // NB, (i + 1) * CR // NB, norm_rows, 0)

    def project(i, store):
        loads[i].wait()
        w = pairs[i][1]
        cols = w.shape[1]
        tile = min(256, cols)
        for c in range(0, cols, tile):
            r = jnp.dot(normed[...], w[:, c : c + tile], preferred_element_type=F32).astype(BF16)
            store(c, tile, r)

    def grouped(write):
        def store(c, tile, r):
            for o in range(0, tile, 2 * HD):
                at = c + o
                write(at // C, at % C, r[:, o : o + 2 * HD])

        return store

    def put_k(gi, col, r):
        kv_send[gi, 0, :, col : col + 2 * HD] = r

    def put_v(gi, col, r):
        kv_send[gi, 1, :, col : col + 2 * HD] = r

    def put_q(gi, col, r):
        q_send[gi, :, col : col + 2 * HD] = r

    def plane(gi, mi):
        return {"sp": gi * M + mi}

    def kv1(dg):
        return pltpu.make_async_remote_copy(
            kv_send.at[lax.rem(g + dg, G)],
            kv_all.at[s],
            kv1_s.at[dg],
            kv_r.at[dg * M],
            device_id=plane(lax.rem(g + dg, G), m),
            device_id_type=MESH,
        )

    def source(dg, dm):
        return lax.rem(g + G - dg, G) * M + lax.rem(m + M - dm, M)

    def kv_in(dg, dm):
        at = kv_all.at[source(dg, dm)]
        return pltpu.make_async_remote_copy(
            at,
            at,
            kv2_s.at[dg * M + dm],
            kv_r.at[dg * M + dm],
            device_id=plane(g, lax.rem(m + 1, M)),
            device_id_type=MESH,
        )

    def kv2(dg, dm):
        at = kv_all.at[source(dg, 0)]
        return pltpu.make_async_remote_copy(
            at,
            at,
            kv2_s.at[dg * M + dm],
            kv_r.at[dg * M + dm],
            device_id=plane(g, lax.rem(m + dm, M)),
            device_id_type=MESH,
        )

    def forward(dg):
        def one(dm, _):
            kv2(dg, dm).start()
            return 0

        lax.fori_loop(1, M, one, 0)

    def q_copy(dg):
        return pltpu.make_async_remote_copy(
            q_send.at[lax.rem(g + dg, G)],
            q_all.at[g],
            q_s.at[dg],
            q_r.at[dg],
            device_id=plane(lax.rem(g + dg, G), m),
            device_id_type=MESH,
        )

    def q_in(dg):
        return pltpu.make_async_remote_copy(
            q_send.at[0],
            q_all.at[lax.rem(g + G - dg, G)],
            q_s.at[dg],
            q_r.at[dg],
            device_id=plane(lax.rem(g + dg, G), m),
            device_id_type=MESH,
        )

    project(0, grouped(put_q))
    for dg in range(1, G):
        q_copy(dg).start()
    q_all[g] = q_send[g]
    project(1, grouped(put_k))
    project(2, grouped(put_v))
    for dg in range(1, G):
        kv1(dg).start()
    kv_all[s] = kv_send[g]
    forward(0)

    def into(ref, first=0):
        def store(c, tile, r):
            ref[first:, c : c + tile] = r

        return store

    project(3, into(band_k, WINDOW))
    project(4, into(band_v, WINDOW))

    def tails():
        nxt = {"sp": lax.rem(s + 1, S)}
        return [
            pltpu.make_async_remote_copy(
                b.at[pl.ds(R, WINDOW)],
                b.at[pl.ds(0, WINDOW)],
                tail_s.at[i],
                tail_r.at[i],
                device_id=nxt,
                device_id_type=MESH,
            )
            for i, b in enumerate((band_k, band_v))
        ]

    @pl.when(s < S - 1)
    def _():
        for cp in tails():
            cp.start()

    @pl.when(s == 0)
    def _():
        band_k[0:WINDOW] = jnp.zeros((WINDOW, band_k.shape[1]), BF16)
        band_v[0:WINDOW] = jnp.zeros((WINDOW, band_v.shape[1]), BF16)

    def relay(dg):
        kv_in(dg, 0).wait_recv()
        forward(dg)

    project(5, into(sq_buf))
    project(6, into(sg_buf))
    project(7, into(pg_buf))

    @pl.when(s > 0)
    def _():
        for cp in tails():
            cp.wait_recv()

    scale = HD**-0.5
    kv_heads = band_k.shape[1] // HD
    group = sq_buf.shape[1] // band_k.shape[1]
    W = WINDOW
    blocks = R // W
    key_i = lax.broadcasted_iota(jnp.int32, (2 * W, group * W), 0)
    qry_i = lax.rem(lax.broadcasted_iota(jnp.int32, (2 * W, group * W), 1), W)
    lane_head = lax.broadcasted_iota(jnp.int32, (1, group * W), 1) // W
    dist = qry_i - key_i + W
    in_band = (dist >= 0) & (dist < W)

    def window_block(b):
        r0 = b * W
        ok = in_band & (s * R + r0 - W + key_i >= 0)
        for h in range(kv_heads):
            k = band_k[r0 : r0 + 2 * W, h * HD : (h + 1) * HD]
            v = band_v[r0 : r0 + 2 * W, h * HD : (h + 1) * HD]
            q = jnp.concatenate(
                [sq_buf[r0 : r0 + W, (h * group + e) * HD : (h * group + e + 1) * HD] for e in range(group)], axis=0
            )
            sc = jnp.where(ok, dot_nt(k, q) * scale, -jnp.inf)
            sk = jnp.full((1, group * W), sink[0, h * group], F32)
            for e in range(1, group):
                sk = jnp.where(lane_head == e, sink[0, h * group + e], sk)
            top = jnp.maximum(jnp.max(sc, axis=0, keepdims=True), sk)
            w = jnp.exp(sc - top)
            den = jnp.sum(w, axis=0, keepdims=True) + jnp.exp(sk - top)
            probs = (w * (1.0 / den)).astype(BF16)
            o = dot_tn(v, probs)
            o = jnp.concatenate([o[:, e * W : (e + 1) * W] for e in range(group)], axis=0).T
            cols = slice(h * group * HD, (h + 1) * group * HD)
            gate = sg_buf[r0 : r0 + W, cols].astype(F32)
            slide_mix[r0 : r0 + W, cols] = (o * silu(gate)).astype(BF16)

    for b in range(blocks):
        window_block(b)
    if G > 1:
        relay(1)

    for dg in range(1, G):
        q_in(dg).wait_recv()
    lane = lax.broadcasted_iota(jnp.int32, (R, 2 * HD), 1)
    for gi in range(G):
        for j in range(Hg):
            q = q_all[gi, :, j * 2 * HD : (j + 1) * 2 * HD].astype(F32) * scale
            q2_buf[gi, j, 0:R, :] = jnp.where(lane < HD, q, 0.0).astype(BF16)
            q2_buf[gi, j, R:, :] = jnp.where(lane < HD, 0.0, q).astype(BF16)
    m_buf[...] = jnp.full(m_buf.shape, -1e30, F32)
    l_buf[...] = jnp.zeros(l_buf.shape, F32)
    acc_buf[...] = jnp.zeros(acc_buf.shape, F32)

    def update(at, gi, masked):
        for j in range(Hg):
            cols = slice(j * 2 * HD, (j + 1) * 2 * HD)
            st = dot_nt(kv_all[at, 0, :, cols], q2_buf[gi, j])
            if masked:
                ki = lax.broadcasted_iota(jnp.int32, (R, 2 * R), 0)
                qi = lax.rem(lax.broadcasted_iota(jnp.int32, (R, 2 * R), 1), R)
                st = jnp.where(qi >= ki, st, -jnp.inf)
            old = m_buf[gi, j]
            new = jnp.maximum(old, jnp.max(st, axis=0, keepdims=True))
            f = jnp.exp(old - new)
            p = jnp.exp(st - new)
            m_buf[gi, j] = new
            l_buf[gi, j] = l_buf[gi, j] * f + jnp.sum(p, axis=0, keepdims=True)
            acc_buf[gi, j] = acc_buf[gi, j] * f + dot_tn(kv_all[at, 1, :, cols], p.astype(BF16))

    def process(at):
        def one(gi, _):
            mine = gi * M + m

            @pl.when(at < mine)
            def _():
                update(at, gi, False)

            @pl.when(at == mine)
            def _():
                update(at, gi, True)

            return 0

        lax.fori_loop(0, G, one, 0)

    def ret_copy(dg):
        return pltpu.make_async_remote_copy(
            ret_send.at[lax.rem(g + dg, G)],
            ret_all.at[g],
            ret_s.at[dg],
            ret_r.at[dg],
            device_id=plane(lax.rem(g + dg, G), m),
            device_id_type=MESH,
        )

    def ret_in(dg):
        return pltpu.make_async_remote_copy(
            ret_send.at[0],
            ret_all.at[lax.rem(g + G - dg, G)],
            ret_s.at[dg],
            ret_r.at[dg],
            device_id=plane(lax.rem(g + dg, G), m),
            device_id_type=MESH,
        )

    def finish(gi):
        for j in range(Hg):
            a = acc_buf[gi, j] * (1.0 / l_buf[gi, j])
            d = a[:, 0:R] - lam[0, g * Hg + j] * a[:, R:]
            sq = jnp.mean(d * d, axis=0, keepdims=True)
            y = (d * (lax.rsqrt(sq + norm_eps) * head_scale)).T * head_gain[...]
            ret_send[gi, :, j * 2 * HD : (j + 1) * 2 * HD] = y.astype(BF16)

    def step(dg, _):
        def far(dm, _):
            kv_in(dg, dm).wait_recv()
            process(source(dg, dm))
            return 0

        half = max(1, M // 2)
        process(source(dg, 0))
        lax.fori_loop(1, half, far, 0)

        @pl.when(dg + 2 < G)
        def _():
            relay(dg + 2)

        lax.fori_loop(half, M, far, 0)

        def close(gi, last):
            last = jnp.maximum(last, lax.rem(g + G - gi, G))

            @pl.when(last == dg)
            def _():
                finish(gi)

                @pl.when(gi != g)
                def _():
                    ret_copy(lax.rem(gi + G - g, G)).start()

            return last

        lax.fori_loop(0, G, close, 0)
        return 0

    lax.fori_loop(0, G, step, 0)
    ret_all[g] = ret_send[g]

    loads[8].wait()
    NT = min(512, D)
    for c in range(0, D, NT):
        part[:, c : c + NT] = jnp.dot(slide_mix[...], wo[:, c : c + NT], preferred_element_type=F32)
    for dg in range(1, G):
        ret_in(dg).wait_recv()
    for gi in range(G):
        gate = pg_buf[:, gi * C : (gi + 1) * C].astype(F32)
        paired_mix[:, gi * C : (gi + 1) * C] = (ret_all[gi].astype(F32) * silu(gate)).astype(BF16)
    loads[9].wait()
    Rt = R // T

    def rs_copy(dt, i):
        cols = pl.ds(i * NT, NT)
        return pltpu.make_async_remote_copy(
            part_bf.at[lax.rem(t + dt, T), :, cols],
            out.at[dt, :, cols],
            rs_s.at[dt, i],
            rs_r.at[dt, i],
            device_id={"tp": lax.rem(t + dt, T)},
            device_id_type=MESH,
        )

    for c in range(0, D, NT):
        r = part[:, c : c + NT] + jnp.dot(paired_mix[...], po[:, c : c + NT], preferred_element_type=F32)
        r = r.astype(BF16)
        for k in range(T):
            part_bf[k, :, c : c + NT] = r[k * Rt : (k + 1) * Rt]
        for dt in range(1, T):
            rs_copy(dt, c // NT).start()
    out[0] = part_bf[t]
    for c in range(0, D, NT):
        for dt in range(1, T):
            rs_copy(dt, c // NT).wait()

    for dt in range(1, T):
        for i in range(TC):
            tok_copy(dt, i).wait_send()
    for dg in range(1, G):
        kv1(dg).wait_send()
        q_copy(dg).wait_send()
        ret_copy(dg).wait_send()

    def drain(i, _):
        kv2(i // (M - 1), 1 + lax.rem(i, M - 1)).wait_send()
        return 0

    if M > 1:
        lax.fori_loop(0, G * (M - 1), drain, 0)

    @pl.when(s < S - 1)
    def _():
        for cp in tails():
            cp.wait_send()


def per_device(S, T, tokens, norm_gain, wq, wk, wv, wg, sink, pq, pk, pv, pg, lam, head_gain, wo, po):
    R, Dl = tokens.shape
    D = Dl * T
    A = wq.shape[1]
    KC = wk.shape[1]
    B = pq.shape[1]
    H = B // (2 * HD)
    G = math.gcd(H, S)
    Hg = H // G
    C = Hg * 2 * HD
    vmem = pl.BlockSpec(memory_space=pltpu.VMEM)
    smem = pl.BlockSpec(memory_space=pltpu.SMEM)
    hbm = pl.BlockSpec(memory_space=pl.ANY)
    dma = pltpu.SemaphoreType.DMA
    V = pltpu.VMEM
    scratch = [V(w.shape, BF16) for w in (wq, wk, wv, wg, pq, pk, pv, pg, wo, po)]
    scratch += [
        V((T, R, Dl), BF16),
        V((R, D), BF16),
        V((WINDOW + R, KC), BF16),
        V((WINDOW + R, KC), BF16),
        V((R, A), BF16),
        V((R, A), BF16),
        V((R, B), BF16),
        V((R, A), BF16),
        V((R, B), BF16),
        V((G, 2, R, C), BF16),
        V((G, R, C), BF16),
        V((S, 2, R, C), BF16),
        V((G, R, C), BF16),
        V((G, Hg, 2 * R, 2 * HD), BF16),
        V((G, Hg, 1, 2 * R), F32),
        V((G, Hg, 1, 2 * R), F32),
        V((G, Hg, 2 * HD, 2 * R), F32),
        V((G, R, C), BF16),
        V((G, R, C), BF16),
        V((R, D), F32),
        V((T, R // T, D), BF16),
        dma((10,)),
        dma((T, 4)),
        dma((T, 4)),
        dma((G,)),
        dma((S,)),
        dma((S,)),
        dma((G,)),
        dma((G,)),
        dma((2,)),
        dma((2,)),
        dma((G,)),
        dma((G,)),
        dma((T, max(1, D // 512))),
        dma((T, max(1, D // 512))),
    ]
    shares = pl.pallas_call(
        functools.partial(kernel, S, T),
        out_shape=jax.ShapeDtypeStruct((T, R // T, D), BF16),
        in_specs=[vmem, vmem, hbm, hbm, hbm, hbm, smem, hbm, hbm, hbm, hbm, smem, vmem, hbm, hbm],
        out_specs=vmem,
        scratch_shapes=scratch,
        compiler_params=pltpu.CompilerParams(
            collective_id=0, has_side_effects=True, vmem_limit_bytes=60 * 1024 * 1024
        ),
        name="layer",
    )(
        tokens,
        norm_gain.reshape(1, D),
        wq,
        wk,
        wv,
        wg,
        sink.reshape(1, -1),
        pq,
        pk,
        pv,
        pg,
        lam.reshape(1, -1),
        head_gain.reshape(1, -1),
        wo,
        po,
    )
    return jnp.sum(shares.astype(F32), axis=0).astype(BF16)


def solution(mesh):
    S, T = mesh.shape["sp"], mesh.shape["tp"]
    in_specs = (
        P("sp", "tp"),
        P(),
        P(None, "tp"),
        P(None, "tp"),
        P(None, "tp"),
        P(None, "tp"),
        P("tp"),
        P(None, "tp"),
        P(None, "tp"),
        P(None, "tp"),
        P(None, "tp"),
        P("tp"),
        P(),
        P("tp", None),
        P("tp", None),
    )
    return jax.shard_map(
        functools.partial(per_device, S, T),
        mesh=mesh,
        in_specs=in_specs,
        out_specs=P(("sp", "tp"), None),
        check_vma=False,
    )
```

```python
import functools
import math

import jax
import jax.numpy as jnp
from jax import lax
from jax.experimental import pallas as pl
from jax.experimental.pallas import tpu as pltpu
from jax.sharding import PartitionSpec as P

HD = 64
WINDOW = 128

norm_eps = 1e-06
head_scale = 0.8

MESH = pl.DeviceIdType.MESH
F32 = jnp.float32
BF16 = jnp.bfloat16


def dot_nt(a, b):
    return lax.dot_general(a, b, (((1,), (1,)), ((), ())), preferred_element_type=F32)


def dot_tn(a, b):
    return lax.dot_general(a, b, (((0,), (0,)), ((), ())), preferred_element_type=F32)


def silu(v):
    return v / (1.0 + jnp.exp(-v))


def kernel(
    S,
    T,
    tokens,
    norm_gain,
    wq_h,
    wk_h,
    wv_h,
    wg_h,
    sink,
    pq_h,
    pk_h,
    pv_h,
    pg_h,
    lam,
    head_gain,
    wo_h,
    po_h,
    out,
    wq,
    wk,
    wv,
    wg,
    pq,
    pk,
    pv,
    pg,
    wo,
    po,
    tok_buf,
    normed,
    band_k,
    band_v,
    sq_buf,
    sg_buf,
    pg_buf,
    slide_mix,
    paired_mix,
    kv_send,
    q_send,
    kv_all,
    q_all,
    q2_buf,
    m_buf,
    l_buf,
    acc_buf,
    ret_send,
    ret_all,
    part,
    part_bf,
    w_sem,
    tok_s,
    tok_r,
    kv1_s,
    kv2_s,
    kv_r,
    q_s,
    q_r,
    tail_s,
    tail_r,
    ret_s,
    ret_r,
    rs_s,
    rs_r,
):
    R = tokens.shape[0]
    Dl = tokens.shape[1]
    D = Dl * T
    G = kv_send.shape[0]
    M = S // G
    C = kv_send.shape[3]
    Hg = C // (2 * HD)
    s = lax.axis_index("sp")
    t = lax.axis_index("tp")
    g = s // M
    m = lax.rem(s, M)

    pairs = [(pq_h, pq), (pk_h, pk), (pv_h, pv), (wk_h, wk), (wv_h, wv), (wq_h, wq), (wg_h, wg), (pg_h, pg), (wo_h, wo), (po_h, po)]
    loads = [pltpu.make_async_copy(a, b, w_sem.at[i]) for i, (a, b) in enumerate(pairs)]
    for cp in loads:
        cp.start()

    barrier = pltpu.get_barrier_semaphore()
    for dt in range(1, T):
        pl.semaphore_signal(barrier, inc=1, device_id={"tp": lax.rem(t + dt, T)}, device_id_type=MESH)

    def greet(d, _):
        pl.semaphore_signal(barrier, inc=1, device_id={"sp": lax.rem(s + d, S)}, device_id_type=MESH)
        return 0

    lax.fori_loop(1, S, greet, 0)
    tok_buf[t] = tokens[...]
    pl.semaphore_wait(barrier, S + T - 2)

    TC = tok_s.shape[1]
    CR = R // TC

    def tok_copy(dt, i):
        return pltpu.make_async_remote_copy(
            tokens.at[pl.ds(i * CR, CR)],
            tok_buf.at[t, pl.ds(i * CR, CR)],
            tok_s.at[dt, i],
            tok_r.at[dt, i],
            device_id={"tp": lax.rem(t + dt, T)},
            device_id_type=MESH,
        )

    def tok_in(dt, i):
        return pltpu.make_async_remote_copy(
            tokens.at[pl.ds(i * CR, CR)],
            tok_buf.at[lax.rem(t + T - dt, T), pl.ds(i * CR, CR)],
            tok_s.at[dt, i],
            tok_r.at[dt, i],
            device_id={"tp": lax.rem(t + dt, T)},
            device_id_type=MESH,
        )

    for i in range(TC):
        for dt in range(1, T):
            tok_copy(dt, i).start()

    NB = 32

    def norm_rows(i, _):
        rows = pl.ds(pl.multiple_of(i * NB, NB), NB)
        xs = [tok_buf[k, rows, :].astype(F32) for k in range(T)]
        total = sum(jnp.sum(x * x, axis=-1, keepdims=True) for x in xs)
        r = lax.rsqrt(total * (1.0 / D) + norm_eps)
        for k in range(T):
            cols = slice(k * Dl, (k + 1) * Dl)
            normed[rows, cols] = (xs[k] * r * norm_gain[:, cols]).astype(BF16)
        return 0

    for i in range(TC):
        for dt in range(1, T):
            tok_in(dt, i).wait_recv()
        lax.fori_loop(i * CR // NB, (i + 1) * CR // NB, norm_rows, 0)

    def project(i, store):
        loads[i].wait()
        w = pairs[i][1]
        cols = w.shape[1]
        tile = min(256, cols)
        for c in range(0, cols, tile):
            r = jnp.dot(normed[...], w[:, c : c + tile], preferred_element_type=F32).astype(BF16)
            store(c, tile, r)

    def grouped(write):
        def store(c, tile, r):
            for o in range(0, tile, 2 * HD):
                at = c + o
                write(at // C, at % C, r[:, o : o + 2 * HD])

        return store

    def put_k(gi, col, r):
        kv_send[gi, 0, :, col : col + 2 * HD] = r

    def put_v(gi, col, r):
        kv_send[gi, 1, :, col : col + 2 * HD] = r

    def put_q(gi, col, r):
        q_send[gi, :, col : col + 2 * HD] = r

    def plane(gi, mi):
        return {"sp": gi * M + mi}

    def kv1(dg):
        return pltpu.make_async_remote_copy(
            kv_send.at[lax.rem(g + dg, G)],
            kv_all.at[s],
            kv1_s.at[dg],
            kv_r.at[dg * M],
            device_id=plane(lax.rem(g + dg, G), m),
            device_id_type=MESH,
        )

    def source(dg, dm):
        return lax.rem(g + G - dg, G) * M + lax.rem(m + M - dm, M)

    def kv_in(dg, dm):
        at = kv_all.at[source(dg, dm)]
        return pltpu.make_async_remote_copy(
            at,
            at,
            kv2_s.at[dg * M + dm],
            kv_r.at[dg * M + dm],
            device_id=plane(g, lax.rem(m + 1, M)),
            device_id_type=MESH,
        )

    def kv2(dg, dm):
        at = kv_all.at[source(dg, 0)]
        return pltpu.make_async_remote_copy(
            at,
            at,
            kv2_s.at[dg * M + dm],
            kv_r.at[dg * M + dm],
            device_id=plane(g, lax.rem(m + dm, M)),
            device_id_type=MESH,
        )

    def forward(dg):
        def one(dm, _):
            kv2(dg, dm).start()
            return 0

        lax.fori_loop(1, M, one, 0)

    def q_copy(dg):
        return pltpu.make_async_remote_copy(
            q_send.at[lax.rem(g + dg, G)],
            q_all.at[g],
            q_s.at[dg],
            q_r.at[dg],
            device_id=plane(lax.rem(g + dg, G), m),
            device_id_type=MESH,
        )

    def q_in(dg):
        return pltpu.make_async_remote_copy(
            q_send.at[0],
            q_all.at[lax.rem(g + G - dg, G)],
            q_s.at[dg],
            q_r.at[dg],
            device_id=plane(lax.rem(g + dg, G), m),
            device_id_type=MESH,
        )

    project(1, grouped(put_k))
    project(2, grouped(put_v))
    for dg in range(1, G):
        kv1(dg).start()
    kv_all[s] = kv_send[g]
    forward(0)
    project(0, grouped(put_q))
    for dg in range(1, G):
        q_copy(dg).start()
    q_all[g] = q_send[g]

    def into(ref, first=0):
        def store(c, tile, r):
            ref[first:, c : c + tile] = r

        return store

    project(3, into(band_k, WINDOW))
    project(4, into(band_v, WINDOW))

    def tails():
        nxt = {"sp": lax.rem(s + 1, S)}
        return [
            pltpu.make_async_remote_copy(
                b.at[pl.ds(R, WINDOW)],
                b.at[pl.ds(0, WINDOW)],
                tail_s.at[i],
                tail_r.at[i],
                device_id=nxt,
                device_id_type=MESH,
            )
            for i, b in enumerate((band_k, band_v))
        ]

    @pl.when(s < S - 1)
    def _():
        for cp in tails():
            cp.start()

    @pl.when(s == 0)
    def _():
        band_k[0:WINDOW] = jnp.zeros((WINDOW, band_k.shape[1]), BF16)
        band_v[0:WINDOW] = jnp.zeros((WINDOW, band_v.shape[1]), BF16)

    def relay(dg):
        kv_in(dg, 0).wait_recv()
        forward(dg)

    project(5, into(sq_buf))
    project(6, into(sg_buf))
    project(7, into(pg_buf))

    @pl.when(s > 0)
    def _():
        for cp in tails():
            cp.wait_recv()

    scale = HD**-0.5
    kv_heads = band_k.shape[1] // HD
    group = sq_buf.shape[1] // band_k.shape[1]
    W = WINDOW
    blocks = R // W
    key_i = lax.broadcasted_iota(jnp.int32, (2 * W, group * W), 0)
    qry_i = lax.rem(lax.broadcasted_iota(jnp.int32, (2 * W, group * W), 1), W)
    lane_head = lax.broadcasted_iota(jnp.int32, (1, group * W), 1) // W
    dist = qry_i - key_i + W
    in_band = (dist >= 0) & (dist < W)

    def window_block(b):
        r0 = b * W
        ok = in_band & (s * R + r0 - W + key_i >= 0)
        for h in range(kv_heads):
            k = band_k[r0 : r0 + 2 * W, h * HD : (h + 1) * HD]
            v = band_v[r0 : r0 + 2 * W, h * HD : (h + 1) * HD]
            q = jnp.concatenate(
                [sq_buf[r0 : r0 + W, (h * group + e) * HD : (h * group + e + 1) * HD] for e in range(group)], axis=0
            )
            sc = jnp.where(ok, dot_nt(k, q) * scale, -jnp.inf)
            sk = jnp.full((1, group * W), sink[0, h * group], F32)
            for e in range(1, group):
                sk = jnp.where(lane_head == e, sink[0, h * group + e], sk)
            top = jnp.maximum(jnp.max(sc, axis=0, keepdims=True), sk)
            w = jnp.exp(sc - top)
            den = jnp.sum(w, axis=0, keepdims=True) + jnp.exp(sk - top)
            probs = (w * (1.0 / den)).astype(BF16)
            o = dot_tn(v, probs)
            o = jnp.concatenate([o[:, e * W : (e + 1) * W] for e in range(group)], axis=0).T
            cols = slice(h * group * HD, (h + 1) * group * HD)
            gate = sg_buf[r0 : r0 + W, cols].astype(F32)
            slide_mix[r0 : r0 + W, cols] = (o * silu(gate)).astype(BF16)

    for b in range(blocks):
        window_block(b)
    if G > 1:
        relay(1)

    for dg in range(1, G):
        q_in(dg).wait_recv()
    lane = lax.broadcasted_iota(jnp.int32, (R, 2 * HD), 1)
    for gi in range(G):
        for j in range(Hg):
            q = q_all[gi, :, j * 2 * HD : (j + 1) * 2 * HD].astype(F32) * scale
            q2_buf[gi, j, 0:R, :] = jnp.where(lane < HD, q, 0.0).astype(BF16)
            q2_buf[gi, j, R:, :] = jnp.where(lane < HD, 0.0, q).astype(BF16)
    m_buf[...] = jnp.full(m_buf.shape, -1e30, F32)
    l_buf[...] = jnp.zeros(l_buf.shape, F32)
    acc_buf[...] = jnp.zeros(acc_buf.shape, F32)

    def update(at, gi, masked):
        for j in range(Hg):
            cols = slice(j * 2 * HD, (j + 1) * 2 * HD)
            st = dot_nt(kv_all[at, 0, :, cols], q2_buf[gi, j])
            if masked:
                ki = lax.broadcasted_iota(jnp.int32, (R, 2 * R), 0)
                qi = lax.rem(lax.broadcasted_iota(jnp.int32, (R, 2 * R), 1), R)
                st = jnp.where(qi >= ki, st, -jnp.inf)
            old = m_buf[gi, j]
            new = jnp.maximum(old, jnp.max(st, axis=0, keepdims=True))
            f = jnp.exp(old - new)
            p = jnp.exp(st - new)
            m_buf[gi, j] = new
            l_buf[gi, j] = l_buf[gi, j] * f + jnp.sum(p, axis=0, keepdims=True)
            acc_buf[gi, j] = acc_buf[gi, j] * f + dot_tn(kv_all[at, 1, :, cols], p.astype(BF16))

    def process(at):
        def one(gi, _):
            mine = gi * M + m

            @pl.when(at < mine)
            def _():
                update(at, gi, False)

            @pl.when(at == mine)
            def _():
                update(at, gi, True)

            return 0

        lax.fori_loop(0, G, one, 0)

    def ret_copy(dg):
        return pltpu.make_async_remote_copy(
            ret_send.at[lax.rem(g + dg, G)],
            ret_all.at[g],
            ret_s.at[dg],
            ret_r.at[dg],
            device_id=plane(lax.rem(g + dg, G), m),
            device_id_type=MESH,
        )

    def ret_in(dg):
        return pltpu.make_async_remote_copy(
            ret_send.at[0],
            ret_all.at[lax.rem(g + G - dg, G)],
            ret_s.at[dg],
            ret_r.at[dg],
            device_id=plane(lax.rem(g + dg, G), m),
            device_id_type=MESH,
        )

    def finish(gi):
        for j in range(Hg):
            a = acc_buf[gi, j] * (1.0 / l_buf[gi, j])
            d = a[:, 0:R] - lam[0, g * Hg + j] * a[:, R:]
            sq = jnp.mean(d * d, axis=0, keepdims=True)
            y = (d * (lax.rsqrt(sq + norm_eps) * head_scale)).T * head_gain[...]
            ret_send[gi, :, j * 2 * HD : (j + 1) * 2 * HD] = y.astype(BF16)

    def step(dg, _):
        def far(dm, _):
            kv_in(dg, dm).wait_recv()
            process(source(dg, dm))
            return 0

        half = max(1, M // 2)
        process(source(dg, 0))
        lax.fori_loop(1, half, far, 0)

        @pl.when(dg + 2 < G)
        def _():
            relay(dg + 2)

        lax.fori_loop(half, M, far, 0)

        def close(gi, last):
            last = jnp.maximum(last, lax.rem(g + G - gi, G))

            @pl.when(last == dg)
            def _():
                finish(gi)

                @pl.when(gi != g)
                def _():
                    ret_copy(lax.rem(gi + G - g, G)).start()

            return last

        lax.fori_loop(0, G, close, 0)
        return 0

    lax.fori_loop(0, G, step, 0)
    ret_all[g] = ret_send[g]

    loads[8].wait()
    NT = min(512, D)
    for c in range(0, D, NT):
        part[:, c : c + NT] = jnp.dot(slide_mix[...], wo[:, c : c + NT], preferred_element_type=F32)
    for dg in range(1, G):
        ret_in(dg).wait_recv()
    for gi in range(G):
        gate = pg_buf[:, gi * C : (gi + 1) * C].astype(F32)
        paired_mix[:, gi * C : (gi + 1) * C] = (ret_all[gi].astype(F32) * silu(gate)).astype(BF16)
    loads[9].wait()
    Rt = R // T

    def rs_copy(dt, i):
        cols = pl.ds(i * NT, NT)
        return pltpu.make_async_remote_copy(
            part_bf.at[lax.rem(t + dt, T), :, cols],
            out.at[dt, :, cols],
            rs_s.at[dt, i],
            rs_r.at[dt, i],
            device_id={"tp": lax.rem(t + dt, T)},
            device_id_type=MESH,
        )

    for c in range(0, D, NT):
        r = part[:, c : c + NT] + jnp.dot(paired_mix[...], po[:, c : c + NT], preferred_element_type=F32)
        r = r.astype(BF16)
        for k in range(T):
            part_bf[k, :, c : c + NT] = r[k * Rt : (k + 1) * Rt]
        for dt in range(1, T):
            rs_copy(dt, c // NT).start()
    out[0] = part_bf[t]
    for c in range(0, D, NT):
        for dt in range(1, T):
            rs_copy(dt, c // NT).wait()

    for dt in range(1, T):
        for i in range(TC):
            tok_copy(dt, i).wait_send()
    for dg in range(1, G):
        kv1(dg).wait_send()
        q_copy(dg).wait_send()
        ret_copy(dg).wait_send()

    def drain(i, _):
        kv2(i // (M - 1), 1 + lax.rem(i, M - 1)).wait_send()
        return 0

    if M > 1:
        lax.fori_loop(0, G * (M - 1), drain, 0)

    @pl.when(s < S - 1)
    def _():
        for cp in tails():
            cp.wait_send()


def per_device(S, T, tokens, norm_gain, wq, wk, wv, wg, sink, pq, pk, pv, pg, lam, head_gain, wo, po):
    R, Dl = tokens.shape
    D = Dl * T
    A = wq.shape[1]
    KC = wk.shape[1]
    B = pq.shape[1]
    H = B // (2 * HD)
    G = math.gcd(H, S)
    Hg = H // G
    C = Hg * 2 * HD
    vmem = pl.BlockSpec(memory_space=pltpu.VMEM)
    smem = pl.BlockSpec(memory_space=pltpu.SMEM)
    hbm = pl.BlockSpec(memory_space=pl.ANY)
    dma = pltpu.SemaphoreType.DMA
    V = pltpu.VMEM
    scratch = [V(w.shape, BF16) for w in (wq, wk, wv, wg, pq, pk, pv, pg, wo, po)]
    scratch += [
        V((T, R, Dl), BF16),
        V((R, D), BF16),
        V((WINDOW + R, KC), BF16),
        V((WINDOW + R, KC), BF16),
        V((R, A), BF16),
        V((R, A), BF16),
        V((R, B), BF16),
        V((R, A), BF16),
        V((R, B), BF16),
        V((G, 2, R, C), BF16),
        V((G, R, C), BF16),
        V((S, 2, R, C), BF16),
        V((G, R, C), BF16),
        V((G, Hg, 2 * R, 2 * HD), BF16),
        V((G, Hg, 1, 2 * R), F32),
        V((G, Hg, 1, 2 * R), F32),
        V((G, Hg, 2 * HD, 2 * R), F32),
        V((G, R, C), BF16),
        V((G, R, C), BF16),
        V((R, D), F32),
        V((T, R // T, D), BF16),
        dma((10,)),
        dma((T, 4)),
        dma((T, 4)),
        dma((G,)),
        dma((S,)),
        dma((S,)),
        dma((G,)),
        dma((G,)),
        dma((2,)),
        dma((2,)),
        dma((G,)),
        dma((G,)),
        dma((T, max(1, D // 512))),
        dma((T, max(1, D // 512))),
    ]
    shares = pl.pallas_call(
        functools.partial(kernel, S, T),
        out_shape=jax.ShapeDtypeStruct((T, R // T, D), BF16),
        in_specs=[vmem, vmem, hbm, hbm, hbm, hbm, smem, hbm, hbm, hbm, hbm, smem, vmem, hbm, hbm],
        out_specs=vmem,
        scratch_shapes=scratch,
        compiler_params=pltpu.CompilerParams(
            collective_id=0, has_side_effects=True, vmem_limit_bytes=60 * 1024 * 1024
        ),
        name="layer",
    )(
        tokens,
        norm_gain.reshape(1, D),
        wq,
        wk,
        wv,
        wg,
        sink.reshape(1, -1),
        pq,
        pk,
        pv,
        pg,
        lam.reshape(1, -1),
        head_gain.reshape(1, -1),
        wo,
        po,
    )
    return jnp.sum(shares.astype(F32), axis=0).astype(BF16)


def solution(mesh):
    S, T = mesh.shape["sp"], mesh.shape["tp"]
    in_specs = (
        P("sp", "tp"),
        P(),
        P(None, "tp"),
        P(None, "tp"),
        P(None, "tp"),
        P(None, "tp"),
        P("tp"),
        P(None, "tp"),
        P(None, "tp"),
        P(None, "tp"),
        P(None, "tp"),
        P("tp"),
        P(),
        P("tp", None),
        P("tp", None),
    )
    return jax.shard_map(
        functools.partial(per_device, S, T),
        mesh=mesh,
        in_specs=in_specs,
        out_specs=P(("sp", "tp"), None),
        check_vma=False,
    )
```
